32 devices in a mesh: ep: 8 (over z, x), tp: 4 (over y, core).
Axes of the slice: x: 2, y: 2, z: 4, core: 2. Of those that a mesh axis runs over, the one named last changes fastest.
Arguments:
- tokens: bfloat16 [2048, 2048], P('ep')
- norm_gain: float32 [2048], replicated, may hold values from 0.1 to 1.9
- chosen: int32 [8, 256], replicated, may hold values from 0 to 2047, as said below
- route_weight: float32 [8, 256], P('ep'), may hold values from 0.2 to 1
- gate_weight: bfloat16 [8, 2048, 4096], P('ep', None, 'tp'), may hold values from -0.125 to 0.125
- up_weight: bfloat16 [8, 2048, 4096], P('ep', None, 'tp'), may hold values from -0.125 to 0.125
- down_weight: bfloat16 [8, 4096, 2048], P('ep', 'tp'), may hold values from -0.09375 to 0.09375
Outputs:
- combined: bfloat16 [2048, 2048], P('ep', 'tp')
The draws below stay inside these ranges and needn't reach their ends.
Inputs may be any that keep to these rules, and one draw needn't show every extreme that they name: Each row of chosen lists 256 distinct token numbers in ascending order. Of the 256 consecutive tokens of one index of ep, a row holds at most 48, and every draw has rows that hold exactly 48 of them.
All inputs are finite; a program needn't handle non-finite values.
Results may differ from the reference program's by a relative error of at most 0.02.
Values may be sent and summed in bfloat16 or wider, within the bound.
A program may use at most 64 MiB of HBM per device.

```python
import math
import jax
import jax.numpy as jnp
from jax import lax

D = 2048
FF = 4096
TOK_DEV = 256
EXPERTS = 8
TOKENS = 2048
CAP = 256
FF_BLK = 1024
N_TP = 4


def draw_tokens(key, part):
    keys = jax.random.split(jax.random.fold_in(key, 11), 3)
    row_scale = jnp.exp(jax.random.uniform(keys[0], (TOKENS, 1), jnp.float32, 0.0, math.log(10.0)))
    col_scale = jnp.exp(jax.random.uniform(keys[1], (1, D), jnp.float32, 0.0, math.log(10.0)))
    values = jax.random.normal(keys[2], (TOKENS, D), jnp.float32)
    return (values * row_scale * col_scale / 3.0).astype(jnp.bfloat16)


def draw_chosen(key, part):
    share = TOK_DEV // 8
    pairs = EXPERTS // 2
    steps = jnp.arange(pairs, dtype=jnp.int32)
    spread = share // 2 * steps // max(pairs - 1, 1)
    base = jnp.stack([share + spread, share - spread], axis=1).reshape(EXPERTS)
    expert_keys = jax.random.split(jax.random.fold_in(key, 23), EXPERTS)

    def one_expert(expert_key):
        order_key, rank_key = jax.random.split(expert_key)
        counts = base[jax.random.permutation(order_key, EXPERTS)]
        block_keys = jax.random.split(rank_key, EXPERTS)
        ranks = jax.vmap(lambda block_key: jax.random.permutation(block_key, TOK_DEV))(block_keys)
        picked = (ranks < counts[:, None]).reshape(TOKENS).astype(jnp.int32)
        order = jnp.argsort(1 - picked, stable=True)
        return order[:CAP].astype(jnp.int32)
    return jax.vmap(one_expert)(expert_keys)


def steps_of(stream_key, extent, cuts, least, top_value):
    def one(dim, blocks):
        heights = jax.random.uniform(jax.random.fold_in(jax.random.fold_in(stream_key, 6), dim), (blocks,), jnp.float32, least / len(cuts), top_value / len(cuts))
        return jnp.repeat(jnp.exp(heights), extent[dim] // blocks).reshape((-1,) + (1,) * (len(extent) - dim - 1))

    gain = one(*cuts[0])
    for cut in cuts[1:]:
        gain = gain * one(*cut)
    return gain


def scatter_about(stream_key, shape, width, reach, pieces=(), kind=jnp.bfloat16):
    array = width * jax.random.normal(stream_key, shape, jnp.float32)
    if pieces:
        array = array * steps_of(stream_key, shape, pieces, -0.22, 0.18)
    return jnp.clip(array, -reach, reach).astype(kind)


def setup_inputs(seed: int = 0) -> dict:
    key_list = jax.random.split(jax.random.key(seed), 8)
    return {
        "tokens": draw_tokens(jax.random.fold_in(key_list[7], 71), 0),
        "norm_gain": jnp.clip(1.0 + 0.18 * jax.random.normal(key_list[1], (D,), jnp.float32), 0.1, 1.9),
        "chosen": draw_chosen(jax.random.fold_in(key_list[7], 71), 0),
        "route_weight": jnp.clip(0.2 + 0.8 * jax.random.uniform(key_list[3], (EXPERTS, CAP), jnp.float32) ** steps_of(key_list[3], (EXPERTS, CAP), ((0, 8),), -0.2, 0.2), 0.2, 1.0),
        "gate_weight": scatter_about(key_list[4], (EXPERTS, D, FF), D ** -0.5, 0.125, ((0, 8), (2, 4))),
        "up_weight": scatter_about(key_list[5], (EXPERTS, D, FF), D ** -0.5, 0.125, ((0, 8), (2, 4))),
        "down_weight": scatter_about(key_list[6], (EXPERTS, FF, D), FF ** -0.5, 0.09375, ((0, 8), (1, 4))),
    }


def normalize(tokens, norm_gain):
    values = tokens.astype(jnp.float32)
    scale = lax.rsqrt(lax.optimization_barrier(jnp.mean(values * values, axis=-1, keepdims=True)) + 1e-06)
    return (values * scale * norm_gain[None, :]).astype(jnp.bfloat16)

def reference(tokens, norm_gain, chosen, route_weight, gate_weight, up_weight, down_weight):
    normed = normalize(tokens, norm_gain)

    def expert_step(combined, inputs):
        token_ids, weights, gate_mat, up_mat, down_mat = inputs
        expert_rows = normed[token_ids]
        gate_pre = jnp.dot(expert_rows, gate_mat, preferred_element_type=jnp.float32)
        up_pre = jnp.dot(expert_rows, up_mat, preferred_element_type=jnp.float32)
        hidden = (jax.nn.silu(gate_pre) * up_pre).astype(jnp.bfloat16)
        hidden_blocks = hidden.reshape(CAP, N_TP, FF_BLK).astype(jnp.float32)
        down_blocks = down_mat.reshape(N_TP, FF_BLK, D).astype(jnp.float32)
        partial_value = jnp.einsum('cnf,nfd->ncd', hidden_blocks, down_blocks).astype(jnp.bfloat16)
        partial_value = lax.optimization_barrier(partial_value)
        summed = lax.optimization_barrier(jnp.sum(partial_value.astype(jnp.float32), axis=0))
        weighted = (weights[:, None] * summed).astype(jnp.bfloat16)
        combined = combined.at[token_ids].add(weighted.astype(jnp.float32))
        return (combined, None)
    start_total = jnp.zeros((TOKENS, D), jnp.float32)
    combined, _ = lax.scan(expert_step, start_total, (chosen, route_weight, gate_weight, up_weight, down_weight))
    return combined.astype(jnp.bfloat16)
```

```python
import functools
import jax
import jax.numpy as jnp
from jax import lax
from jax.experimental import pallas as pl
from jax.experimental.pallas import tpu as pltpu
from jax.sharding import PartitionSpec as P

F32 = jnp.float32
BF16 = jnp.bfloat16
MESH = pl.DeviceIdType.MESH
SHARES = (1, 1, 1)
CUTS_IN = ((1, 1), (1, 1), (1, 1))
CUTS_OUT = ((1,), (1,), (1,))
CUTS_BACK = ((1, 1), (1, 1), (1, 1))

def shards(tokens, norm_gain, chosen, route_weight, gate_weight, up_weight, down_weight):
    tok_rows, row_width = tokens.shape
    experts, capacity = chosen.shape
    ep_count = lax.axis_size("ep")
    tp_count = lax.axis_size("tp")
    owner_index = lax.axis_index("ep")
    slot_most = 3 * tok_rows // 16
    col_width = row_width // tp_count
    values = tokens.astype(jnp.float32)
    scale = lax.rsqrt(jnp.mean(values * values, axis=-1, keepdims=True) + 1e-06)
    normed = (values * scale * norm_gain[None, :]).astype(jnp.bfloat16)
    slot_steps = jnp.arange(slot_most, dtype=jnp.int32)
    first_token = owner_index * tok_rows
    run_start = jnp.sum((chosen < first_token).astype(jnp.int32), axis=1)
    run_end = jnp.sum((chosen < first_token + tok_rows).astype(jnp.int32), axis=1)
    run_count = run_end - run_start
    slot_live = slot_steps[None, :] < run_count[:, None]
    slot_place = jnp.minimum(run_start[:, None] + slot_steps[None, :], capacity - 1)
    slot_token = jnp.take_along_axis(chosen, slot_place, axis=1) - first_token
    slot_local = jnp.where(slot_live, slot_token, 0)
    my_chosen = lax.dynamic_index_in_dim(chosen, owner_index, 0, keepdims=False)
    block_edges = jnp.arange(ep_count, dtype=jnp.int32) * tok_rows
    src_start = jnp.sum((my_chosen[None, :] < block_edges[:, None]).astype(jnp.int32), axis=1)
    src_end = jnp.concatenate([src_start[1:], jnp.full((1,), capacity, jnp.int32)])
    gate_mat = gate_weight[0]
    up_mat = up_weight[0]
    down_mat = down_weight[0]
    outgoing = jnp.where(slot_live[:, :, None], normed[slot_local], jnp.zeros((), jnp.bfloat16))
    received = lax.all_to_all(outgoing, "ep", split_axis=0, concat_axis=0, tiled=True)
    source_block = my_chosen // tok_rows
    flat_index = (
        source_block * slot_most + jnp.arange(capacity, dtype=jnp.int32) - src_start[source_block]
    )
    expert_rows = received.reshape(-1, row_width)[flat_index]
    gate_pre = jnp.dot(expert_rows, gate_mat, preferred_element_type=jnp.float32)
    up_pre = jnp.dot(expert_rows, up_mat, preferred_element_type=jnp.float32)
    hidden = (jax.nn.silu(gate_pre) * up_pre).astype(jnp.bfloat16)
    summed_out = lax.psum_scatter(
        lax.dot_general(
            down_mat, hidden, (((0,), (1,)), ((), ())), preferred_element_type=jnp.float32
        ).astype(jnp.bfloat16),
        "tp",
        scatter_dimension=0,
        tiled=True,
    ).astype(jnp.float32)
    weighted = (summed_out.T * route_weight[0][:, None]).astype(jnp.bfloat16)
    back_place = jnp.minimum(src_start[:, None] + slot_steps[None, :], capacity - 1)
    back_live = slot_steps[None, :] < (src_end - src_start)[:, None]
    outgoing_back = jnp.where(
        back_live[:, :, None], weighted[back_place], jnp.zeros((), jnp.bfloat16)
    )
    returned = lax.all_to_all(outgoing_back, "ep", split_axis=0, concat_axis=0, tiled=True)
    target_row = jnp.where(slot_live, slot_token, tok_rows).reshape(-1)
    placement = (jnp.arange(tok_rows, dtype=jnp.int32)[:, None] == target_row[None, :]).astype(
        jnp.bfloat16
    )
    combined = jnp.dot(
        placement, returned.reshape(-1, col_width), preferred_element_type=jnp.float32
    )
    return combined.astype(jnp.bfloat16)


def cut(total, shares):
    sizes = [total * s // sum(shares) for s in shares]
    return [(sum(sizes[:i]), size) for i, size in enumerate(sizes)]


def group_rows(cap, slots, ep, first, count):
    most = max(min(m * count, cap - m * first) for m in range(1, ep + 1))
    return min(-(-most // 16) * 16, ep * count)


def fused_kernel(
    ep, groups, rows_of, cuts_in, cuts_out, cuts_back,
    tokens_hbm, gain_hbm, chosen_hbm, route_hbm, gate_hbm, up_hbm, down_hbm, out,
    tokens, gain, chosen, route,
    gate_w, up_w, down_w, normed, pick, unpick, spread, gather, weight, gate_acc, up_acc, hidden,
    outgoing, received, rows, pair_out, pair_in, own_part, cross_out, cross_in, back_out, back_in, done,
    in_sem, w_sem, send_sem, ep_recv, y_recv, pair_recv, relay_recv, ps_recv, ys_recv, back_recv,
):
    me = lax.axis_index("ep")
    tp = lax.axis_index("tp")
    y_pos = tp // 2
    core = tp % 2
    mate = y_pos * 2 + (1 - core)
    across = (1 - y_pos) * 2 + core
    diag = (1 - y_pos) * 2 + (1 - core)
    tok_rows, width = tokens.shape
    cap = chosen.shape[1]
    quarter = width // 4
    ff = gate_w.shape[1]
    n_groups = len(groups)
    slots = sum(n for _, n in groups)

    if ep & (ep - 1):
        peers = [(me + d) % ep for d in sorted(range(1, ep), key=lambda d: abs(d - ep / 2))]
    else:
        bits = [1 << i for i in range(ep.bit_length() - 1)]

        def flip(mask):
            dest = me
            for b in bits:
                if mask & b:
                    dest = dest + b * (1 - 2 * (me // b % 2))
            return dest

        peers = [flip(m) for m in range(ep - 1, 0, -1)]

    small = [
        pltpu.make_async_copy(a, b, in_sem.at[i])
        for i, (a, b) in enumerate(
            [(chosen_hbm, chosen), (tokens_hbm, tokens), (gain_hbm, gain), (route_hbm, route)]
        )
    ]
    for load in small:
        load.start()
    barrier = pltpu.get_barrier_semaphore()
    for dest in peers:
        pl.semaphore_signal(barrier, inc=1, device_id={"ep": dest, "tp": tp}, device_id_type=MESH)
    for other in (mate, across):
        pl.semaphore_signal(barrier, inc=1, device_id={"ep": me, "tp": other}, device_id_type=MESH)

    loads = [
        pltpu.make_async_copy(gate_hbm.at[0], gate_w, w_sem.at[0]),
        pltpu.make_async_copy(up_hbm.at[0], up_w, w_sem.at[1]),
        pltpu.make_async_copy(down_hbm.at[0], down_w, w_sem.at[2]),
    ]
    small[0].wait()

    first = me * tok_rows
    lane = lax.broadcasted_iota(jnp.int32, (slots, cap), 1).astype(F32)
    sub = lax.broadcasted_iota(jnp.int32, (slots, cap), 0).astype(F32)
    tok_lane = lax.broadcasted_iota(jnp.int32, (slots, tok_rows), 1).astype(F32)
    for e in range(ep):
        row = chosen[e : e + 1, :]
        local = (row - first).astype(F32)
        start = jnp.sum(jnp.where(local < 0.0, 1.0, 0.0), axis=1, keepdims=True)
        value = jnp.where((local >= 0.0) & (local < float(tok_rows)), local + 1.0, 0.0)
        hit = lane == sub + start
        slot_tok = jnp.sum(jnp.where(hit, value, 0.0), axis=1, keepdims=True) - 1.0
        one = jnp.where(tok_lane == slot_tok, 1.0, 0.0)
        for g, (s0, n) in enumerate(groups):
            pick[g][e * n : (e + 1) * n, :] = one[s0 : s0 + n]

    for load in small[1:]:
        load.wait()
    my_cols = pl.ds(pl.multiple_of(tp * quarter, quarter), quarter)
    my_gain = gain[:, my_cols]
    step_rows = 32
    for r in range(0, tok_rows, step_rows):
        rs = pl.ds(r, step_rows)
        v = tokens[rs, :].astype(F32)
        scale = lax.rsqrt(jnp.sum(v * v, axis=1, keepdims=True) * (1.0 / width) + 1e-06)
        own = tokens[rs, my_cols].astype(F32)
        normed[rs, :] = (own * scale * my_gain).astype(BF16)

    def ep_copies(buf_out, buf_in, n, r_sem):
        return [
            pltpu.make_async_remote_copy(
                src_ref=buf_out.at[pl.ds(pl.multiple_of(dest * n, 8), n)],
                dst_ref=buf_in.at[pl.ds(pl.multiple_of(me * n, 8), n)],
                send_sem=send_sem.at[0], recv_sem=r_sem,
                device_id={"ep": dest, "tp": tp}, device_id_type=MESH,
            )
            for dest in peers
        ]

    def tp_copy(a, b, r_sem, other):
        return pltpu.make_async_remote_copy(
            src_ref=a, dst_ref=b, send_sem=send_sem.at[0], recv_sem=r_sem,
            device_id={"ep": me, "tp": other}, device_id_type=MESH,
        )

    sent = []

    def go(c, size):
        c.start()
        sent.append(size)

    def landed(buf, n, sem):
        part = buf.at[pl.ds(0, n)]
        pltpu.make_async_copy(part, part, sem).wait()

    def mine_rows(n):
        return pl.ds(pl.multiple_of(me * n, 8), n)

    def send_in(g, k):
        n = groups[g][1]
        off, size = cuts_in[g][k]
        got = jnp.dot(
            pick[g][...].astype(BF16), normed[:, off : off + size], preferred_element_type=F32
        )
        outgoing[g][k][...] = got.astype(BF16)

    def start_in(g, k):
        n = groups[g][1]
        for c in ep_copies(outgoing[g][k], received[g][k], n, ep_recv[g].at[k]):
            go(c, n * cuts_in[g][k][1])
        received[g][k][mine_rows(n), :] = outgoing[g][k][mine_rows(n), :]

    send_in(0, 0)
    pl.semaphore_wait(barrier, ep + 1)
    start_in(0, 0)
    for k in range(1, len(cuts_in[0])):
        send_in(0, k)
        start_in(0, k)
    for load in loads:
        load.start()

    for g in range(1, n_groups):
        for k in range(len(cuts_in[g])):
            send_in(g, k)

    mine = chosen[pl.ds(me, 1), :].astype(F32)
    place = lax.broadcasted_iota(jnp.int32, (1, cap), 1).astype(F32)
    rank = jnp.zeros((1, cap), F32)
    block = jnp.zeros((1, cap), F32)
    edges = [(mine >= float(b * tok_rows)) & (mine < float((b + 1) * tok_rows)) for b in range(ep)]
    for b in range(ep):
        begin = jnp.sum(jnp.where(mine < float(b * tok_rows), 1.0, 0.0), axis=1, keepdims=True)
        rank = jnp.where(edges[b], place - begin, rank)
        block = jnp.where(edges[b], float(b), block)
    for g, (s0, n) in enumerate(groups):
        inside = (rank >= float(s0)) & (rank < float(s0 + n))
        slot_of = jnp.where(inside, block * float(n) + rank - float(s0), -1.0)
        slot_sub = lax.broadcasted_iota(jnp.int32, (ep * n, cap), 0).astype(F32)
        slot_hot = slot_sub == slot_of
        if rows_of[g] == ep * n:
            row_hot = slot_hot
        else:
            row_id = jnp.zeros((1, cap), F32)
            for b in range(ep):
                below = jnp.where(inside & (mine < float(b * tok_rows)), 1.0, 0.0)
                shift = jnp.sum(below, axis=1, keepdims=True) - float(s0)
                row_id = jnp.where(edges[b], rank + shift, row_id)
            row_id = jnp.where(inside, row_id, -1.0)
            row_sub = lax.broadcasted_iota(jnp.int32, (rows_of[g], cap), 0).astype(F32)
            row_hot = row_sub == row_id
            slot_b = jnp.where(slot_hot, 1.0, 0.0).astype(BF16)
            row_b = jnp.where(row_hot, 1.0, 0.0).astype(BF16)
            across_lanes = (((1,), (1,)), ((), ()))
            spread[g][...] = lax.dot_general(
                slot_b, row_b, across_lanes, preferred_element_type=F32
            ).astype(BF16)
            gather[g][...] = lax.dot_general(
                row_b, slot_b, across_lanes, preferred_element_type=F32
            ).astype(BF16)
        weight[g][...] = jnp.sum(jnp.where(row_hot, route[...], 0.0), axis=1, keepdims=True)
        unpick[g][...] = pick[g][...].T.astype(BF16)

    def start_on(side, *chunks):
        @pl.when(core == side)
        def _():
            for g, k in chunks:
                n = groups[g][1]
                for c in ep_copies(outgoing[g][k], received[g][k], n, ep_recv[g].at[k]):
                    c.start()
                    if side:
                        sent.append(n * cuts_in[g][k][1])
                received[g][k][mine_rows(n), :] = outgoing[g][k][mine_rows(n), :]

    def recv(g, k):
        n = groups[g][1]
        landed(received[g][k], (ep - 1) * n, ep_recv[g].at[k])
        mine_k = rows[g][k].at[tp]
        if rows_of[g] == ep * n:
            mine_k[...] = received[g][k][...]
        else:
            got = jnp.dot(gather[g][...], received[g][k][...], preferred_element_type=F32)
            mine_k[...] = got.astype(BF16)
        size = rows_of[g] * cuts_in[g][k][1]
        go(tp_copy(mine_k, mine_k, y_recv[g].at[k], across), size)
        go(tp_copy(mine_k, mine_k, pair_recv[g].at[k], mate), size)

    def relay(g, k):
        there = rows[g][k].at[across]
        tp_copy(there, there, y_recv[g].at[k], across).wait_recv()
        go(tp_copy(there, there, relay_recv[g].at[k], mate), rows_of[g] * cuts_in[g][k][1])

    def project(g, near, far, opening=False, closing=False):
        for k in near:
            there = rows[g][k].at[mate]
            tp_copy(there, there, pair_recv[g].at[k], mate).wait_recv()
        for k in far:
            there = rows[g][k].at[diag]
            tp_copy(there, there, relay_recv[g].at[k], mate).wait_recv()
        work = [(k, t) for k in near for t in (tp, mate)] + [(k, t) for k in far for t in (across, diag)]
        tile = 256
        for n in range(0, ff, tile):
            cols = pl.ds(n, tile)
            gg = None if opening else gate_acc[g][:, cols]
            uu = None if opening else up_acc[g][:, cols]
            for k, t in work:
                off, size = cuts_in[g][k]
                ks = pl.ds(pl.multiple_of(t * quarter + off, 128), size)
                x = rows[g][k][t]
                dg = jnp.dot(x, gate_w[ks, cols], preferred_element_type=F32)
                du = jnp.dot(x, up_w[ks, cols], preferred_element_type=F32)
                gg = dg if gg is None else gg + dg
                uu = du if uu is None else uu + du
            if closing:
                hidden[g][:, cols] = (gg / (1.0 + jnp.exp(-gg)) * uu).astype(BF16)
            else:
                gate_acc[g][:, cols] = gg
                up_acc[g][:, cols] = uu

    def down(g, t, j):
        off, size = cuts_out[g][j]
        cols = pl.ds(pl.multiple_of(t * quarter + off, 128), size)
        return jnp.dot(hidden[g][...], down_w[:, cols], preferred_element_type=F32)

    def pair_copy(g, j, half):
        return tp_copy(pair_out[g][j].at[half], pair_in[g][j].at[half], ps_recv[g].at[j, half], mate)

    def give(g, j):
        for half, t in enumerate((diag, mate)):
            pair_out[g][j][half] = down(g, t, j).astype(BF16)
            go(pair_copy(g, j, half), rows_of[g] * cuts_out[g][j][1])

    def keep(g, j, which):
        own_part[g][j][which] = down(g, tp if which else across, j)

    def piece(g, i):
        off, size = cuts_back[g][i]
        for j, (base, wide) in enumerate(cuts_out[g]):
            if base <= off < base + wide:
                return j, slice(off - base, off - base + size)

    def cross(g, i):
        j, part = piece(g, i)
        if part.start == 0:
            pair_copy(g, j, 0).wait_recv()
        kept = own_part[g][j][0, :, part] + pair_in[g][j][0, :, part].astype(F32)
        cross_out[g][i][...] = kept.astype(BF16)
        go(tp_copy(cross_out[g][i], cross_in[g][i], ys_recv[g].at[i], across), rows_of[g] * cuts_back[g][i][1])

    def back(g, i):
        n = groups[g][1]
        j, part = piece(g, i)
        if part.start == 0:
            pair_copy(g, j, 1).wait_recv()
        near = own_part[g][j][1, :, part] + pair_in[g][j][1, :, part].astype(F32)
        tp_copy(cross_out[g][i], cross_in[g][i], ys_recv[g].at[i], across).wait_recv()
        total = ((near + cross_in[g][i][...].astype(F32)) * weight[g][...]).astype(BF16)
        if rows_of[g] == ep * n:
            back_out[g][i][...] = total
        else:
            wide = jnp.dot(spread[g][...], total, preferred_element_type=F32)
            back_out[g][i][...] = wide.astype(BF16)
        for c in ep_copies(back_out[g][i], back_in[g][i], n, back_recv[g].at[i]):
            go(c, n * cuts_back[g][i][1])
        back_in[g][i][mine_rows(n), :] = back_out[g][i][mine_rows(n), :]

    def finish(g, i):
        n = groups[g][1]
        off, size = cuts_back[g][i]
        landed(back_in[g][i], (ep - 1) * n, back_recv[g].at[i])
        part = jnp.dot(unpick[g][...], back_in[g][i][...], preferred_element_type=F32)
        if g:
            part = part + done[:, off : off + size]
        if g == n_groups - 1:
            out[:, off : off + size] = part.astype(BF16)
        else:
            done[:, off : off + size] = part

    def weights(i):
        loads[i].wait()

    start_on(0, (1, 0), (1, 1))
    recv(0, 0)
    start_on(1, (1, 0), (1, 1))
    recv(0, 1)
    start_on(0, (2, 0), (2, 1))
    weights(0)
    weights(1)
    project(0, [0, 1], [], opening=True)
    recv(1, 0)
    start_on(1, (2, 0), (2, 1))
    relay(0, 0)
    recv(1, 1)
    relay(0, 1)
    project(0, [], [0, 1], closing=True)
    weights(2)
    give(0, 0)
    recv(2, 0)
    relay(1, 0)
    keep(0, 0, 0)
    recv(2, 1)
    relay(1, 1)
    project(1, [1], [], opening=True)
    cross(0, 0)
    project(1, [0], [0])
    cross(0, 1)
    project(1, [], [1], closing=True)
    give(1, 0)
    relay(2, 1)
    relay(2, 0)
    keep(0, 0, 1)
    keep(1, 0, 1)
    project(2, [0], [], opening=True)
    keep(1, 0, 0)
    cross(1, 0)
    cross(1, 1)
    project(2, [], [0])
    back(0, 0)
    project(2, [1], [1], closing=True)
    give(2, 0)
    back(0, 1)
    keep(2, 0, 0)
    cross(2, 0)
    back(1, 0)
    back(1, 1)
    keep(2, 0, 1)
    finish(0, 0)
    cross(2, 1)
    finish(0, 1)
    back(2, 0)
    back(2, 1)
    finish(1, 0)
    finish(1, 1)
    finish(2, 0)
    finish(2, 1)

    words = sum(sent)
    rest = pl.ds(0, words // ff)
    pltpu.make_async_copy(gate_w.at[rest], gate_w.at[rest], send_sem.at[0]).wait()


def fused(tokens, norm_gain, chosen, route_weight, gate_weight, up_weight, down_weight):
    ep = lax.axis_size("ep")
    tok_rows, width = tokens.shape
    cap = chosen.shape[1]
    slots = 3 * tok_rows // 16
    quarter = width // lax.axis_size("tp")
    ff = gate_weight.shape[2]
    groups = cut(slots, SHARES)
    rows_of = [group_rows(cap, slots, ep, s0, n) for s0, n in groups]
    cuts_in = [cut(quarter, c) for c in CUTS_IN]
    cuts_out = [cut(quarter, c) for c in CUTS_OUT]
    cuts_back = [cut(quarter, c) for c in CUTS_BACK]
    hbm = pl.BlockSpec(memory_space=pl.ANY)
    dma = pltpu.SemaphoreType.DMA
    wide = [ep * n for _, n in groups]

    def bufs(cuts, lead, dtype=BF16):
        return [[pltpu.VMEM(lead(g) + (size,), dtype) for _, size in c] for g, c in enumerate(cuts)]

    def each(shape, dtype=BF16):
        return [pltpu.VMEM(shape(g), dtype) for g in range(len(groups))]

    def sems(cuts):
        return [dma((len(c),)) for c in cuts]

    return pl.pallas_call(
        functools.partial(fused_kernel, ep, groups, rows_of, cuts_in, cuts_out, cuts_back),
        out_shape=pltpu.VMEM((tok_rows, quarter), BF16),
        in_specs=[hbm] * 7,
        out_specs=pl.BlockSpec(memory_space=pltpu.VMEM),
        scratch_shapes=[
            pltpu.VMEM((tok_rows, width), BF16),
            pltpu.VMEM((1, width), F32),
            pltpu.VMEM(chosen.shape, jnp.int32),
            pltpu.VMEM((1, cap), F32),
            pltpu.VMEM((width, ff), BF16),
            pltpu.VMEM((width, ff), BF16),
            pltpu.VMEM((ff, width), BF16),
            pltpu.VMEM((tok_rows, quarter), BF16),
            each(lambda g: (wide[g], tok_rows), F32),
            each(lambda g: (tok_rows, wide[g])),
            each(lambda g: (wide[g], rows_of[g])),
            each(lambda g: (rows_of[g], wide[g])),
            each(lambda g: (rows_of[g], 1), F32),
            each(lambda g: (rows_of[g], ff), F32),
            each(lambda g: (rows_of[g], ff), F32),
            each(lambda g: (rows_of[g], ff)),
            bufs(cuts_in, lambda g: (wide[g],)),
            bufs(cuts_in, lambda g: (wide[g],)),
            bufs(cuts_in, lambda g: (4, rows_of[g])),
            bufs(cuts_out, lambda g: (2, rows_of[g])),
            bufs(cuts_out, lambda g: (2, rows_of[g])),
            bufs(cuts_out, lambda g: (2, rows_of[g]), F32),
            bufs(cuts_back, lambda g: (rows_of[g],)),
            bufs(cuts_back, lambda g: (rows_of[g],)),
            bufs(cuts_back, lambda g: (wide[g],)),
            bufs(cuts_back, lambda g: (wide[g],)),
            pltpu.VMEM((tok_rows, quarter), F32),
            dma((4,)),
            dma((3,)),
            dma((1,)),
            sems(cuts_in),
            sems(cuts_in),
            sems(cuts_in),
            sems(cuts_in),
            [dma((len(c), 2)) for c in cuts_out],
            sems(cuts_back),
            sems(cuts_back),
        ],
        compiler_params=pltpu.CompilerParams(
            collective_id=0, has_side_effects=True, vmem_limit_bytes=60 * 1024 * 1024
        ),
    )(tokens, norm_gain[None, :], chosen, route_weight, gate_weight, up_weight, down_weight)


def solution(mesh):
    small = mesh.shape["tp"] == 4
    return jax.shard_map(
        fused if small else shards,
        mesh=mesh,
        in_specs=(
            P("ep", None),
            P(),
            P(),
            P("ep", None),
            P("ep", None, "tp"),
            P("ep", None, "tp"),
            P("ep", "tp", None),
        ),
        out_specs=P("ep", "tp"),
        check_vma=False,
    )
```

```python
import functools
import jax
import jax.numpy as jnp
from jax import lax
from jax.experimental import pallas as pl
from jax.experimental.pallas import tpu as pltpu
from jax.sharding import PartitionSpec as P

F32 = jnp.float32
BF16 = jnp.bfloat16
MESH = pl.DeviceIdType.MESH
SHARES = (1, 1, 1)
CUTS_IN = ((1, 1), (1, 1), (1, 1))
CUTS_OUT = ((1,), (1,), (1,))
CUTS_BACK = ((1, 1), (1, 1), (1, 1))

def shards(tokens, norm_gain, chosen, route_weight, gate_weight, up_weight, down_weight):
    tok_rows, row_width = tokens.shape
    experts, capacity = chosen.shape
    ep_count = lax.axis_size("ep")
    tp_count = lax.axis_size("tp")
    owner_index = lax.axis_index("ep")
    slot_most = 3 * tok_rows // 16
    col_width = row_width // tp_count
    values = tokens.astype(jnp.float32)
    scale = lax.rsqrt(jnp.mean(values * values, axis=-1, keepdims=True) + 1e-06)
    normed = (values * scale * norm_gain[None, :]).astype(jnp.bfloat16)
    slot_steps = jnp.arange(slot_most, dtype=jnp.int32)
    first_token = owner_index * tok_rows
    run_start = jnp.sum((chosen < first_token).astype(jnp.int32), axis=1)
    run_end = jnp.sum((chosen < first_token + tok_rows).astype(jnp.int32), axis=1)
    run_count = run_end - run_start
    slot_live = slot_steps[None, :] < run_count[:, None]
    slot_place = jnp.minimum(run_start[:, None] + slot_steps[None, :], capacity - 1)
    slot_token = jnp.take_along_axis(chosen, slot_place, axis=1) - first_token
    slot_local = jnp.where(slot_live, slot_token, 0)
    my_chosen = lax.dynamic_index_in_dim(chosen, owner_index, 0, keepdims=False)
    block_edges = jnp.arange(ep_count, dtype=jnp.int32) * tok_rows
    src_start = jnp.sum((my_chosen[None, :] < block_edges[:, None]).astype(jnp.int32), axis=1)
    src_end = jnp.concatenate([src_start[1:], jnp.full((1,), capacity, jnp.int32)])
    gate_mat = gate_weight[0]
    up_mat = up_weight[0]
    down_mat = down_weight[0]
    outgoing = jnp.where(slot_live[:, :, None], normed[slot_local], jnp.zeros((), jnp.bfloat16))
    received = lax.all_to_all(outgoing, "ep", split_axis=0, concat_axis=0, tiled=True)
    source_block = my_chosen // tok_rows
    flat_index = (
        source_block * slot_most + jnp.arange(capacity, dtype=jnp.int32) - src_start[source_block]
    )
    expert_rows = received.reshape(-1, row_width)[flat_index]
    gate_pre = jnp.dot(expert_rows, gate_mat, preferred_element_type=jnp.float32)
    up_pre = jnp.dot(expert_rows, up_mat, preferred_element_type=jnp.float32)
    hidden = (jax.nn.silu(gate_pre) * up_pre).astype(jnp.bfloat16)
    summed_out = lax.psum_scatter(
        lax.dot_general(
            down_mat, hidden, (((0,), (1,)), ((), ())), preferred_element_type=jnp.float32
        ).astype(jnp.bfloat16),
        "tp",
        scatter_dimension=0,
        tiled=True,
    ).astype(jnp.float32)
    weighted = (summed_out.T * route_weight[0][:, None]).astype(jnp.bfloat16)
    back_place = jnp.minimum(src_start[:, None] + slot_steps[None, :], capacity - 1)
    back_live = slot_steps[None, :] < (src_end - src_start)[:, None]
    outgoing_back = jnp.where(
        back_live[:, :, None], weighted[back_place], jnp.zeros((), jnp.bfloat16)
    )
    returned = lax.all_to_all(outgoing_back, "ep", split_axis=0, concat_axis=0, tiled=True)
    target_row = jnp.where(slot_live, slot_token, tok_rows).reshape(-1)
    placement = (jnp.arange(tok_rows, dtype=jnp.int32)[:, None] == target_row[None, :]).astype(
        jnp.bfloat16
    )
    combined = jnp.dot(
        placement, returned.reshape(-1, col_width), preferred_element_type=jnp.float32
    )
    return combined.astype(jnp.bfloat16)


def cut(total, shares):
    sizes = [total * s // sum(shares) for s in shares]
    return [(sum(sizes[:i]), size) for i, size in enumerate(sizes)]


def group_rows(cap, slots, ep, first, count):
    most = max(min(m * count, cap - m * first) for m in range(1, ep + 1))
    return min(-(-most // 16) * 16, ep * count)


def fused_kernel(
    ep, groups, rows_of, cuts_in, cuts_out, cuts_back,
    tokens_hbm, gain_hbm, chosen_hbm, route_hbm, gate_hbm, up_hbm, down_hbm, out,
    tokens, gain, chosen, route,
    gate_w, up_w, down_w, normed, pick, unpick, spread, gather, weight, gate_acc, up_acc, hidden,
    outgoing, received, rows, pair_out, pair_in, own_part, cross_out, cross_in, back_out, back_in, done,
    in_sem, w_sem, send_sem, ep_recv, y_recv, pair_recv, relay_recv, ps_recv, ys_recv, back_recv,
):
    me = lax.axis_index("ep")
    tp = lax.axis_index("tp")
    y_pos = tp // 2
    core = tp % 2
    mate = y_pos * 2 + (1 - core)
    across = (1 - y_pos) * 2 + core
    diag = (1 - y_pos) * 2 + (1 - core)
    tok_rows, width = tokens.shape
    cap = chosen.shape[1]
    quarter = width // 4
    ff = gate_w.shape[1]
    n_groups = len(groups)
    slots = sum(n for _, n in groups)

    if ep & (ep - 1):
        peers = [(me + d) % ep for d in sorted(range(1, ep), key=lambda d: abs(d - ep / 2))]
    else:
        bits = [1 << i for i in range(ep.bit_length() - 1)]

        def flip(mask):
            dest = me
            for b in bits:
                if mask & b:
                    dest = dest + b * (1 - 2 * (me // b % 2))
            return dest

        peers = [flip(m) for m in range(ep - 1, 0, -1)]

    top_half, low_half = pl.ds(0, tok_rows // 2), pl.ds(tok_rows // 2, tok_rows // 2)
    small = [
        pltpu.make_async_copy(a, b, in_sem.at[i])
        for i, (a, b) in enumerate(
            [
                (chosen_hbm, chosen),
                (tokens_hbm.at[top_half], tokens.at[top_half]),
                (gain_hbm, gain),
                (tokens_hbm.at[low_half], tokens.at[low_half]),
                (route_hbm, route),
            ]
        )
    ]
    for load in small:
        load.start()
    barrier = pltpu.get_barrier_semaphore()
    for dest in peers:
        pl.semaphore_signal(barrier, inc=1, device_id={"ep": dest, "tp": tp}, device_id_type=MESH)
    for other in (mate, across):
        pl.semaphore_signal(barrier, inc=1, device_id={"ep": me, "tp": other}, device_id_type=MESH)

    loads = [
        pltpu.make_async_copy(gate_hbm.at[0], gate_w, w_sem.at[0]),
        pltpu.make_async_copy(up_hbm.at[0], up_w, w_sem.at[1]),
        pltpu.make_async_copy(down_hbm.at[0], down_w, w_sem.at[2]),
    ]
    small[0].wait()

    first = me * tok_rows
    lane = lax.broadcasted_iota(jnp.int32, (slots, cap), 1).astype(F32)
    sub = lax.broadcasted_iota(jnp.int32, (slots, cap), 0).astype(F32)
    tok_lane = lax.broadcasted_iota(jnp.int32, (slots, tok_rows), 1).astype(F32)
    for e in range(ep):
        row = chosen[e : e + 1, :]
        local = (row - first).astype(F32)
        start = jnp.sum(jnp.where(local < 0.0, 1.0, 0.0), axis=1, keepdims=True)
        value = jnp.where((local >= 0.0) & (local < float(tok_rows)), local + 1.0, 0.0)
        hit = lane == sub + start
        slot_tok = jnp.sum(jnp.where(hit, value, 0.0), axis=1, keepdims=True) - 1.0
        one = jnp.where(tok_lane == slot_tok, 1.0, 0.0)
        for g, (s0, n) in enumerate(groups):
            pick[g][e * n : (e + 1) * n, :] = one[s0 : s0 + n]

    for load in small[1:3]:
        load.wait()
    my_cols = pl.ds(pl.multiple_of(tp * quarter, quarter), quarter)
    my_gain = gain[:, my_cols]
    step_rows = 32
    for r in range(0, tok_rows, step_rows):
        if r == tok_rows // 2:
            for load in small[3:]:
                load.wait()
        rs = pl.ds(r, step_rows)
        v = tokens[rs, :].astype(F32)
        scale = lax.rsqrt(jnp.sum(v * v, axis=1, keepdims=True) * (1.0 / width) + 1e-06)
        own = tokens[rs, my_cols].astype(F32)
        normed[rs, :] = (own * scale * my_gain).astype(BF16)

    def ep_copies(buf_out, buf_in, n, r_sem):
        return [
            pltpu.make_async_remote_copy(
                src_ref=buf_out.at[pl.ds(pl.multiple_of(dest * n, 8), n)],
                dst_ref=buf_in.at[pl.ds(pl.multiple_of(me * n, 8), n)],
                send_sem=send_sem.at[0], recv_sem=r_sem,
                device_id={"ep": dest, "tp": tp}, device_id_type=MESH,
            )
            for dest in peers
        ]

    def tp_copy(a, b, r_sem, other):
        return pltpu.make_async_remote_copy(
            src_ref=a, dst_ref=b, send_sem=send_sem.at[0], recv_sem=r_sem,
            device_id={"ep": me, "tp": other}, device_id_type=MESH,
        )

    sent = []

    def go(c, size):
        c.start()
        sent.append(size)

    def landed(buf, n, sem):
        part = buf.at[pl.ds(0, n)]
        pltpu.make_async_copy(part, part, sem).wait()

    def mine_rows(n):
        return pl.ds(pl.multiple_of(me * n, 8), n)

    def send_in(g, k):
        n = groups[g][1]
        off, size = cuts_in[g][k]
        got = jnp.dot(
            pick[g][...].astype(BF16), normed[:, off : off + size], preferred_element_type=F32
        )
        outgoing[g][k][...] = got.astype(BF16)

    def start_in(g, k):
        n = groups[g][1]
        for c in ep_copies(outgoing[g][k], received[g][k], n, ep_recv[g].at[k]):
            go(c, n * cuts_in[g][k][1])
        received[g][k][mine_rows(n), :] = outgoing[g][k][mine_rows(n), :]

    send_in(0, 0)
    pl.semaphore_wait(barrier, ep + 1)
    start_in(0, 0)
    for k in range(1, len(cuts_in[0])):
        send_in(0, k)
        start_in(0, k)
    for load in loads:
        load.start()

    for g in range(1, n_groups):
        for k in range(len(cuts_in[g])):
            send_in(g, k)

    mine = chosen[pl.ds(me, 1), :].astype(F32)
    place = lax.broadcasted_iota(jnp.int32, (1, cap), 1).astype(F32)
    rank = jnp.zeros((1, cap), F32)
    block = jnp.zeros((1, cap), F32)
    edges = [(mine >= float(b * tok_rows)) & (mine < float((b + 1) * tok_rows)) for b in range(ep)]
    for b in range(ep):
        begin = jnp.sum(jnp.where(mine < float(b * tok_rows), 1.0, 0.0), axis=1, keepdims=True)
        rank = jnp.where(edges[b], place - begin, rank)
        block = jnp.where(edges[b], float(b), block)
    for g, (s0, n) in enumerate(groups):
        inside = (rank >= float(s0)) & (rank < float(s0 + n))
        slot_of = jnp.where(inside, block * float(n) + rank - float(s0), -1.0)
        slot_sub = lax.broadcasted_iota(jnp.int32, (ep * n, cap), 0).astype(F32)
        slot_hot = slot_sub == slot_of
        if rows_of[g] == ep * n:
            row_hot = slot_hot
        else:
            row_id = jnp.zeros((1, cap), F32)
            for b in range(ep):
                below = jnp.where(inside & (mine < float(b * tok_rows)), 1.0, 0.0)
                shift = jnp.sum(below, axis=1, keepdims=True) - float(s0)
                row_id = jnp.where(edges[b], rank + shift, row_id)
            row_id = jnp.where(inside, row_id, -1.0)
            row_sub = lax.broadcasted_iota(jnp.int32, (rows_of[g], cap), 0).astype(F32)
            row_hot = row_sub == row_id
            slot_b = jnp.where(slot_hot, 1.0, 0.0).astype(BF16)
            row_b = jnp.where(row_hot, 1.0, 0.0).astype(BF16)
            across_lanes = (((1,), (1,)), ((), ()))
            spread[g][...] = lax.dot_general(
                slot_b, row_b, across_lanes, preferred_element_type=F32
            ).astype(BF16)
            gather[g][...] = lax.dot_general(
                row_b, slot_b, across_lanes, preferred_element_type=F32
            ).astype(BF16)
        weight[g][...] = jnp.sum(jnp.where(row_hot, route[...], 0.0), axis=1, keepdims=True)
        unpick[g][...] = pick[g][...].T.astype(BF16)

    def start_on(side, *chunks):
        @pl.when(core == side)
        def _():
            for g, k in chunks:
                n = groups[g][1]
                for c in ep_copies(outgoing[g][k], received[g][k], n, ep_recv[g].at[k]):
                    c.start()
                    if side:
                        sent.append(n * cuts_in[g][k][1])
                received[g][k][mine_rows(n), :] = outgoing[g][k][mine_rows(n), :]

    def recv(g, k):
        n = groups[g][1]
        landed(received[g][k], (ep - 1) * n, ep_recv[g].at[k])
        mine_k = rows[g][k].at[tp]
        if rows_of[g] == ep * n:
            mine_k[...] = received[g][k][...]
        else:
            got = jnp.dot(gather[g][...], received[g][k][...], preferred_element_type=F32)
            mine_k[...] = got.astype(BF16)
        size = rows_of[g] * cuts_in[g][k][1]
        go(tp_copy(mine_k, mine_k, y_recv[g].at[k], across), size)
        go(tp_copy(mine_k, mine_k, pair_recv[g].at[k], mate), size)

    def relay(g, k):
        there = rows[g][k].at[across]
        tp_copy(there, there, y_recv[g].at[k], across).wait_recv()
        go(tp_copy(there, there, relay_recv[g].at[k], mate), rows_of[g] * cuts_in[g][k][1])

    def project(g, near, far, opening=False, closing=False):
        for k in near:
            there = rows[g][k].at[mate]
            tp_copy(there, there, pair_recv[g].at[k], mate).wait_recv()
        for k in far:
            there = rows[g][k].at[diag]
            tp_copy(there, there, relay_recv[g].at[k], mate).wait_recv()
        work = [(k, t) for k in near for t in (tp, mate)] + [(k, t) for k in far for t in (across, diag)]
        tile = 256
        for n in range(0, ff, tile):
            cols = pl.ds(n, tile)
            gg = None if opening else gate_acc[g][:, cols]
            uu = None if opening else up_acc[g][:, cols]
            for k, t in work:
                off, size = cuts_in[g][k]
                ks = pl.ds(pl.multiple_of(t * quarter + off, 128), size)
                x = rows[g][k][t]
                dg = jnp.dot(x, gate_w[ks, cols], preferred_element_type=F32)
                du = jnp.dot(x, up_w[ks, cols], preferred_element_type=F32)
                gg = dg if gg is None else gg + dg
                uu = du if uu is None else uu + du
            if closing:
                hidden[g][:, cols] = (gg / (1.0 + jnp.exp(-gg)) * uu).astype(BF16)
            else:
                gate_acc[g][:, cols] = gg
                up_acc[g][:, cols] = uu

    def down(g, t, j):
        off, size = cuts_out[g][j]
        cols = pl.ds(pl.multiple_of(t * quarter + off, 128), size)
        return jnp.dot(hidden[g][...], down_w[:, cols], preferred_element_type=F32)

    def pair_copy(g, j, half):
        return tp_copy(pair_out[g][j].at[half], pair_in[g][j].at[half], ps_recv[g].at[j, half], mate)

    def give(g, j):
        parts = [down(g, t, j) for t in (diag, mate)]
        for half, part in enumerate(parts):
            pair_out[g][j][half] = part.astype(BF16)
            go(pair_copy(g, j, half), rows_of[g] * cuts_out[g][j][1])

    def keep(g, j):
        parts = [down(g, t, j) for t in (across, tp)]
        for which, part in enumerate(parts):
            own_part[g][j][which] = part

    def piece(g, i):
        off, size = cuts_back[g][i]
        for j, (base, wide) in enumerate(cuts_out[g]):
            if base <= off < base + wide:
                return j, slice(off - base, off - base + size)

    def cross(g, i):
        j, part = piece(g, i)
        if part.start == 0:
            pair_copy(g, j, 0).wait_recv()
        kept = own_part[g][j][0, :, part] + pair_in[g][j][0, :, part].astype(F32)
        cross_out[g][i][...] = kept.astype(BF16)
        go(tp_copy(cross_out[g][i], cross_in[g][i], ys_recv[g].at[i], across), rows_of[g] * cuts_back[g][i][1])

    def back(g, i):
        n = groups[g][1]
        j, part = piece(g, i)
        if part.start == 0:
            pair_copy(g, j, 1).wait_recv()
        near = own_part[g][j][1, :, part] + pair_in[g][j][1, :, part].astype(F32)
        tp_copy(cross_out[g][i], cross_in[g][i], ys_recv[g].at[i], across).wait_recv()
        total = ((near + cross_in[g][i][...].astype(F32)) * weight[g][...]).astype(BF16)
        if rows_of[g] == ep * n:
            back_out[g][i][...] = total
        else:
            wide = jnp.dot(spread[g][...], total, preferred_element_type=F32)
            back_out[g][i][...] = wide.astype(BF16)
        for c in ep_copies(back_out[g][i], back_in[g][i], n, back_recv[g].at[i]):
            go(c, n * cuts_back[g][i][1])
        back_in[g][i][mine_rows(n), :] = back_out[g][i][mine_rows(n), :]

    def finish(g, i):
        n = groups[g][1]
        off, size = cuts_back[g][i]
        landed(back_in[g][i], (ep - 1) * n, back_recv[g].at[i])
        part = jnp.dot(unpick[g][...], back_in[g][i][...], preferred_element_type=F32)
        if g:
            part = part + done[:, off : off + size]
        if g == n_groups - 1:
            out[:, off : off + size] = part.astype(BF16)
        else:
            done[:, off : off + size] = part

    def weights(i):
        loads[i].wait()

    start_on(0, (1, 0), (1, 1))
    recv(0, 0)
    start_on(1, (1, 0), (1, 1))
    recv(0, 1)
    start_on(0, (2, 0), (2, 1))
    weights(0)
    weights(1)
    project(0, [1], [], opening=True)
    recv(1, 0)
    start_on(1, (2, 0), (2, 1))
    project(0, [0], [])
    recv(1, 1)
    relay(0, 0)
    relay(0, 1)
    project(1, [0], [], opening=True)
    project(0, [], [0, 1], closing=True)
    recv(2, 0)
    weights(2)
    give(0, 0)
    recv(2, 1)
    relay(1, 0)
    keep(0, 0)
    relay(1, 1)
    cross(0, 0)
    project(1, [1], [0])
    cross(0, 1)
    project(1, [], [1], closing=True)
    give(1, 0)
    relay(2, 1)
    relay(2, 0)
    project(2, [1], [], opening=True)
    keep(1, 0)
    cross(1, 0)
    cross(1, 1)
    back(0, 0)
    project(2, [0], [0, 1], closing=True)
    give(2, 0)
    back(0, 1)
    keep(2, 0)
    cross(2, 0)
    back(1, 0)
    back(1, 1)
    cross(2, 1)
    back(2, 0)
    back(2, 1)
    finish(0, 0)
    finish(0, 1)
    finish(1, 0)
    finish(1, 1)
    finish(2, 0)
    finish(2, 1)

    words = sum(sent)
    rest = pl.ds(0, words // ff)
    pltpu.make_async_copy(gate_w.at[rest], gate_w.at[rest], send_sem.at[0]).wait()


def fused(tokens, norm_gain, chosen, route_weight, gate_weight, up_weight, down_weight):
    ep = lax.axis_size("ep")
    tok_rows, width = tokens.shape
    cap = chosen.shape[1]
    slots = 3 * tok_rows // 16
    quarter = width // lax.axis_size("tp")
    ff = gate_weight.shape[2]
    groups = cut(slots, SHARES)
    rows_of = [group_rows(cap, slots, ep, s0, n) for s0, n in groups]
    cuts_in = [cut(quarter, c) for c in CUTS_IN]
    cuts_out = [cut(quarter, c) for c in CUTS_OUT]
    cuts_back = [cut(quarter, c) for c in CUTS_BACK]
    hbm = pl.BlockSpec(memory_space=pl.ANY)
    dma = pltpu.SemaphoreType.DMA
    wide = [ep * n for _, n in groups]

    def bufs(cuts, lead, dtype=BF16):
        return [[pltpu.VMEM(lead(g) + (size,), dtype) for _, size in c] for g, c in enumerate(cuts)]

    def each(shape, dtype=BF16):
        return [pltpu.VMEM(shape(g), dtype) for g in range(len(groups))]

    def sems(cuts):
        return [dma((len(c),)) for c in cuts]

    return pl.pallas_call(
        functools.partial(fused_kernel, ep, groups, rows_of, cuts_in, cuts_out, cuts_back),
        out_shape=pltpu.VMEM((tok_rows, quarter), BF16),
        in_specs=[hbm] * 7,
        out_specs=pl.BlockSpec(memory_space=pltpu.VMEM),
        scratch_shapes=[
            pltpu.VMEM((tok_rows, width), BF16),
            pltpu.VMEM((1, width), F32),
            pltpu.VMEM(chosen.shape, jnp.int32),
            pltpu.VMEM((1, cap), F32),
            pltpu.VMEM((width, ff), BF16),
            pltpu.VMEM((width, ff), BF16),
            pltpu.VMEM((ff, width), BF16),
            pltpu.VMEM((tok_rows, quarter), BF16),
            each(lambda g: (wide[g], tok_rows), F32),
            each(lambda g: (tok_rows, wide[g])),
            each(lambda g: (wide[g], rows_of[g])),
            each(lambda g: (rows_of[g], wide[g])),
            each(lambda g: (rows_of[g], 1), F32),
            each(lambda g: (rows_of[g], ff), F32),
            each(lambda g: (rows_of[g], ff), F32),
            each(lambda g: (rows_of[g], ff)),
            bufs(cuts_in, lambda g: (wide[g],)),
            bufs(cuts_in, lambda g: (wide[g],)),
            bufs(cuts_in, lambda g: (4, rows_of[g])),
            bufs(cuts_out, lambda g: (2, rows_of[g])),
            bufs(cuts_out, lambda g: (2, rows_of[g])),
            bufs(cuts_out, lambda g: (2, rows_of[g]), F32),
            bufs(cuts_back, lambda g: (rows_of[g],)),
            bufs(cuts_back, lambda g: (rows_of[g],)),
            bufs(cuts_back, lambda g: (wide[g],)),
            bufs(cuts_back, lambda g: (wide[g],)),
            pltpu.VMEM((tok_rows, quarter), F32),
            dma((5,)),
            dma((3,)),
            dma((1,)),
            sems(cuts_in),
            sems(cuts_in),
            sems(cuts_in),
            sems(cuts_in),
            [dma((len(c), 2)) for c in cuts_out],
            sems(cuts_back),
            sems(cuts_back),
        ],
        compiler_params=pltpu.CompilerParams(
            collective_id=0, has_side_effects=True, vmem_limit_bytes=60 * 1024 * 1024
        ),
    )(tokens, norm_gain[None, :], chosen, route_weight, gate_weight, up_weight, down_weight)


def solution(mesh):
    small = mesh.shape["tp"] == 4
    return jax.shard_map(
        fused if small else shards,
        mesh=mesh,
        in_specs=(
            P("ep", None),
            P(),
            P(),
            P("ep", None),
            P("ep", None, "tp"),
            P("ep", None, "tp"),
            P("ep", "tp", None),
        ),
        out_specs=P("ep", "tp"),
        check_vma=False,
    )
```

```python
import functools
import jax
import jax.numpy as jnp
from jax import lax
from jax.experimental import pallas as pl
from jax.experimental.pallas import tpu as pltpu
from jax.sharding import PartitionSpec as P

F32 = jnp.float32
BF16 = jnp.bfloat16
MESH = pl.DeviceIdType.MESH
SHARES = (1, 1, 1)
CUTS_IN = ((1, 1), (1, 1), (1, 1))
CUTS_OUT = ((1,), (1,), (1,))
CUTS_BACK = ((1, 1), (1, 1), (1, 1))

def shards(tokens, norm_gain, chosen, route_weight, gate_weight, up_weight, down_weight):
    tok_rows, row_width = tokens.shape
    experts, capacity = chosen.shape
    ep_count = lax.axis_size("ep")
    tp_count = lax.axis_size("tp")
    owner_index = lax.axis_index("ep")
    slot_most = 3 * tok_rows // 16
    col_width = row_width // tp_count
    values = tokens.astype(jnp.float32)
    scale = lax.rsqrt(jnp.mean(values * values, axis=-1, keepdims=True) + 1e-06)
    normed = (values * scale * norm_gain[None, :]).astype(jnp.bfloat16)
    slot_steps = jnp.arange(slot_most, dtype=jnp.int32)
    first_token = owner_index * tok_rows
    run_start = jnp.sum((chosen < first_token).astype(jnp.int32), axis=1)
    run_end = jnp.sum((chosen < first_token + tok_rows).astype(jnp.int32), axis=1)
    run_count = run_end - run_start
    slot_live = slot_steps[None, :] < run_count[:, None]
    slot_place = jnp.minimum(run_start[:, None] + slot_steps[None, :], capacity - 1)
    slot_token = jnp.take_along_axis(chosen, slot_place, axis=1) - first_token
    slot_local = jnp.where(slot_live, slot_token, 0)
    my_chosen = lax.dynamic_index_in_dim(chosen, owner_index, 0, keepdims=False)
    block_edges = jnp.arange(ep_count, dtype=jnp.int32) * tok_rows
    src_start = jnp.sum((my_chosen[None, :] < block_edges[:, None]).astype(jnp.int32), axis=1)
    src_end = jnp.concatenate([src_start[1:], jnp.full((1,), capacity, jnp.int32)])
    gate_mat = gate_weight[0]
    up_mat = up_weight[0]
    down_mat = down_weight[0]
    outgoing = jnp.where(slot_live[:, :, None], normed[slot_local], jnp.zeros((), jnp.bfloat16))
    received = lax.all_to_all(outgoing, "ep", split_axis=0, concat_axis=0, tiled=True)
    source_block = my_chosen // tok_rows
    flat_index = (
        source_block * slot_most + jnp.arange(capacity, dtype=jnp.int32) - src_start[source_block]
    )
    expert_rows = received.reshape(-1, row_width)[flat_index]
    gate_pre = jnp.dot(expert_rows, gate_mat, preferred_element_type=jnp.float32)
    up_pre = jnp.dot(expert_rows, up_mat, preferred_element_type=jnp.float32)
    hidden = (jax.nn.silu(gate_pre) * up_pre).astype(jnp.bfloat16)
    summed_out = lax.psum_scatter(
        lax.dot_general(
            down_mat, hidden, (((0,), (1,)), ((), ())), preferred_element_type=jnp.float32
        ).astype(jnp.bfloat16),
        "tp",
        scatter_dimension=0,
        tiled=True,
    ).astype(jnp.float32)
    weighted = (summed_out.T * route_weight[0][:, None]).astype(jnp.bfloat16)
    back_place = jnp.minimum(src_start[:, None] + slot_steps[None, :], capacity - 1)
    back_live = slot_steps[None, :] < (src_end - src_start)[:, None]
    outgoing_back = jnp.where(
        back_live[:, :, None], weighted[back_place], jnp.zeros((), jnp.bfloat16)
    )
    returned = lax.all_to_all(outgoing_back, "ep", split_axis=0, concat_axis=0, tiled=True)
    target_row = jnp.where(slot_live, slot_token, tok_rows).reshape(-1)
    placement = (jnp.arange(tok_rows, dtype=jnp.int32)[:, None] == target_row[None, :]).astype(
        jnp.bfloat16
    )
    combined = jnp.dot(
        placement, returned.reshape(-1, col_width), preferred_element_type=jnp.float32
    )
    return combined.astype(jnp.bfloat16)


def cut(total, shares):
    sizes = [total * s // sum(shares) for s in shares]
    return [(sum(sizes[:i]), size) for i, size in enumerate(sizes)]


def group_rows(cap, slots, ep, first, count):
    most = max(min(m * count, cap - m * first) for m in range(1, ep + 1))
    return min(-(-most // 16) * 16, ep * count)


def fused_kernel(
    ep, groups, rows_of, cuts_in, cuts_out, cuts_back,
    tokens_hbm, gain_hbm, chosen_hbm, route_hbm, gate_hbm, up_hbm, down_hbm, out,
    tokens, gain, chosen, route,
    gate_w, up_w, down_w, normed, pick, unpick, spread, gather, weight, gate_acc, up_acc, hidden,
    outgoing, received, rows, pair_out, pair_in, own_part, cross_out, cross_in, back_out, back_in, done,
    in_sem, w_sem, send_sem, ep_recv, y_recv, pair_recv, relay_recv, ps_recv, ys_recv, back_recv,
):
    me = lax.axis_index("ep")
    tp = lax.axis_index("tp")
    y_pos = tp // 2
    core = tp % 2
    mate = y_pos * 2 + (1 - core)
    across = (1 - y_pos) * 2 + core
    diag = (1 - y_pos) * 2 + (1 - core)
    tok_rows, width = tokens.shape
    cap = chosen.shape[1]
    quarter = width // 4
    ff = gate_w.shape[1]
    n_groups = len(groups)
    slots = sum(n for _, n in groups)

    if ep & (ep - 1):
        peers = [(me + d) % ep for d in sorted(range(1, ep), key=lambda d: abs(d - ep / 2))]
    else:
        bits = [1 << i for i in range(ep.bit_length() - 1)]

        def flip(mask):
            dest = me
            for b in bits:
                if mask & b:
                    dest = dest + b * (1 - 2 * (me // b % 2))
            return dest

        peers = [flip(m) for m in range(ep - 1, 0, -1)]

    barrier = pltpu.get_barrier_semaphore()
    for dest in peers:
        pl.semaphore_signal(barrier, inc=1, device_id={"ep": dest, "tp": tp}, device_id_type=MESH)
    for other in (mate, across):
        pl.semaphore_signal(barrier, inc=1, device_id={"ep": me, "tp": other}, device_id_type=MESH)

    load_rows = tok_rows // 4
    strips = [pl.ds(i * load_rows, load_rows) for i in range(4)]
    small = [
        pltpu.make_async_copy(a, b, in_sem.at[i])
        for i, (a, b) in enumerate(
            [(chosen_hbm, chosen)]
            + [(tokens_hbm.at[strip], tokens.at[strip]) for strip in strips]
            + [(gain_hbm, gain), (route_hbm, route)]
        )
    ]
    for load in small:
        load.start()
    loads = [
        pltpu.make_async_copy(gate_hbm.at[0], gate_w, w_sem.at[0]),
        pltpu.make_async_copy(up_hbm.at[0], up_w, w_sem.at[1]),
        pltpu.make_async_copy(down_hbm.at[0], down_w, w_sem.at[2]),
    ]
    small[0].wait()

    first = me * tok_rows
    lane = lax.broadcasted_iota(jnp.int32, (slots, cap), 1).astype(F32)
    sub = lax.broadcasted_iota(jnp.int32, (slots, cap), 0).astype(F32)
    tok_lane = lax.broadcasted_iota(jnp.int32, (slots, tok_rows), 1).astype(F32)
    for e in range(ep):
        row = chosen[e : e + 1, :]
        local = (row - first).astype(F32)
        start = jnp.sum(jnp.where(local < 0.0, 1.0, 0.0), axis=1, keepdims=True)
        value = jnp.where((local >= 0.0) & (local < float(tok_rows)), local + 1.0, 0.0)
        hit = lane == sub + start
        slot_tok = jnp.sum(jnp.where(hit, value, 0.0), axis=1, keepdims=True) - 1.0
        one = jnp.where(tok_lane == slot_tok, 1.0, 0.0)
        for g, (s0, n) in enumerate(groups):
            pick[g][e * n : (e + 1) * n, :] = one[s0 : s0 + n]

    for load in small[5:]:
        load.wait()
    my_cols = pl.ds(pl.multiple_of(tp * quarter, quarter), quarter)
    my_gain = gain[:, my_cols]
    step_rows = 32
    for r in range(0, tok_rows, step_rows):
        if r % load_rows == 0:
            small[1 + r // load_rows].wait()
        rs = pl.ds(r, step_rows)
        v = tokens[rs, :].astype(F32)
        scale = lax.rsqrt(jnp.sum(v * v, axis=1, keepdims=True) * (1.0 / width) + 1e-06)
        own = tokens[rs, my_cols].astype(F32)
        normed[rs, :] = (own * scale * my_gain).astype(BF16)

    def ep_copies(buf_out, buf_in, n, r_sem):
        return [
            pltpu.make_async_remote_copy(
                src_ref=buf_out.at[pl.ds(pl.multiple_of(dest * n, 8), n)],
                dst_ref=buf_in.at[pl.ds(pl.multiple_of(me * n, 8), n)],
                send_sem=send_sem.at[0], recv_sem=r_sem,
                device_id={"ep": dest, "tp": tp}, device_id_type=MESH,
            )
            for dest in peers
        ]

    def tp_copy(a, b, r_sem, other):
        return pltpu.make_async_remote_copy(
            src_ref=a, dst_ref=b, send_sem=send_sem.at[0], recv_sem=r_sem,
            device_id={"ep": me, "tp": other}, device_id_type=MESH,
        )

    sent = []

    def go(c, size):
        c.start()
        sent.append(size)

    def landed(buf, n, sem):
        part = buf.at[pl.ds(0, n)]
        pltpu.make_async_copy(part, part, sem).wait()

    def mine_rows(n):
        return pl.ds(pl.multiple_of(me * n, 8), n)

    def send_in(g, k):
        n = groups[g][1]
        off, size = cuts_in[g][k]
        got = jnp.dot(
            pick[g][...].astype(BF16), normed[:, off : off + size], preferred_element_type=F32
        )
        outgoing[g][k][...] = got.astype(BF16)

    def start_in(g, k):
        n = groups[g][1]
        for c in ep_copies(outgoing[g][k], received[g][k], n, ep_recv[g].at[k]):
            go(c, n * cuts_in[g][k][1])
        received[g][k][mine_rows(n), :] = outgoing[g][k][mine_rows(n), :]

    send_in(0, 0)
    pl.semaphore_wait(barrier, ep + 1)
    start_in(0, 0)
    for k in range(1, len(cuts_in[0])):
        send_in(0, k)
        start_in(0, k)
    for load in loads:
        load.start()

    for g in range(1, n_groups):
        for k in range(len(cuts_in[g])):
            send_in(g, k)

    mine = chosen[pl.ds(me, 1), :].astype(F32)
    place = lax.broadcasted_iota(jnp.int32, (1, cap), 1).astype(F32)
    rank = jnp.zeros((1, cap), F32)
    block = jnp.zeros((1, cap), F32)
    edges = [(mine >= float(b * tok_rows)) & (mine < float((b + 1) * tok_rows)) for b in range(ep)]
    for b in range(ep):
        begin = jnp.sum(jnp.where(mine < float(b * tok_rows), 1.0, 0.0), axis=1, keepdims=True)
        rank = jnp.where(edges[b], place - begin, rank)
        block = jnp.where(edges[b], float(b), block)
    for g, (s0, n) in enumerate(groups):
        inside = (rank >= float(s0)) & (rank < float(s0 + n))
        slot_of = jnp.where(inside, block * float(n) + rank - float(s0), -1.0)
        slot_sub = lax.broadcasted_iota(jnp.int32, (ep * n, cap), 0).astype(F32)
        slot_hot = slot_sub == slot_of
        if rows_of[g] == ep * n:
            row_hot = slot_hot
        else:
            row_id = jnp.zeros((1, cap), F32)
            for b in range(ep):
                below = jnp.where(inside & (mine < float(b * tok_rows)), 1.0, 0.0)
                shift = jnp.sum(below, axis=1, keepdims=True) - float(s0)
                row_id = jnp.where(edges[b], rank + shift, row_id)
            row_id = jnp.where(inside, row_id, -1.0)
            row_sub = lax.broadcasted_iota(jnp.int32, (rows_of[g], cap), 0).astype(F32)
            row_hot = row_sub == row_id
            slot_b = jnp.where(slot_hot, 1.0, 0.0).astype(BF16)
            row_b = jnp.where(row_hot, 1.0, 0.0).astype(BF16)
            across_lanes = (((1,), (1,)), ((), ()))
            spread[g][...] = lax.dot_general(
                slot_b, row_b, across_lanes, preferred_element_type=F32
            ).astype(BF16)
            gather[g][...] = lax.dot_general(
                row_b, slot_b, across_lanes, preferred_element_type=F32
            ).astype(BF16)
        weight[g][...] = jnp.sum(jnp.where(row_hot, route[...], 0.0), axis=1, keepdims=True)
        unpick[g][...] = pick[g][...].T.astype(BF16)

    def start_on(side, *chunks):
        @pl.when(core == side)
        def _():
            for g, k in chunks:
                n = groups[g][1]
                for c in ep_copies(outgoing[g][k], received[g][k], n, ep_recv[g].at[k]):
                    c.start()
                    if side:
                        sent.append(n * cuts_in[g][k][1])
                received[g][k][mine_rows(n), :] = outgoing[g][k][mine_rows(n), :]

    def recv(g, k):
        n = groups[g][1]
        landed(received[g][k], (ep - 1) * n, ep_recv[g].at[k])
        mine_k = rows[g][k].at[tp]
        if rows_of[g] == ep * n:
            mine_k[...] = received[g][k][...]
        else:
            got = jnp.dot(gather[g][...], received[g][k][...], preferred_element_type=F32)
            mine_k[...] = got.astype(BF16)
        size = rows_of[g] * cuts_in[g][k][1]
        go(tp_copy(mine_k, mine_k, y_recv[g].at[k], across), size)
        go(tp_copy(mine_k, mine_k, pair_recv[g].at[k], mate), size)

    def relay(g, k):
        there = rows[g][k].at[across]
        tp_copy(there, there, y_recv[g].at[k], across).wait_recv()
        go(tp_copy(there, there, relay_recv[g].at[k], mate), rows_of[g] * cuts_in[g][k][1])

    def project(g, near, far, opening=False, closing=False):
        for k in near:
            there = rows[g][k].at[mate]
            tp_copy(there, there, pair_recv[g].at[k], mate).wait_recv()
        for k in far:
            there = rows[g][k].at[diag]
            tp_copy(there, there, relay_recv[g].at[k], mate).wait_recv()
        work = [(k, t) for k in near for t in (tp, mate)] + [(k, t) for k in far for t in (across, diag)]
        tile = 256
        for n in range(0, ff, tile):
            cols = pl.ds(n, tile)
            gg = None if opening else gate_acc[g][:, cols]
            uu = None if opening else up_acc[g][:, cols]
            for k, t in work:
                off, size = cuts_in[g][k]
                ks = pl.ds(pl.multiple_of(t * quarter + off, 128), size)
                x = rows[g][k][t]
                dg = jnp.dot(x, gate_w[ks, cols], preferred_element_type=F32)
                du = jnp.dot(x, up_w[ks, cols], preferred_element_type=F32)
                gg = dg if gg is None else gg + dg
                uu = du if uu is None else uu + du
            if closing:
                hidden[g][:, cols] = (gg / (1.0 + jnp.exp(-gg)) * uu).astype(BF16)
            else:
                gate_acc[g][:, cols] = gg
                up_acc[g][:, cols] = uu

    def down(g, t, j):
        off, size = cuts_out[g][j]
        cols = pl.ds(pl.multiple_of(t * quarter + off, 128), size)
        return jnp.dot(hidden[g][...], down_w[:, cols], preferred_element_type=F32)

    def pair_copy(g, j, half):
        return tp_copy(pair_out[g][j].at[half], pair_in[g][j].at[half], ps_recv[g].at[j, half], mate)

    def give(g, j):
        parts = [down(g, t, j) for t in (diag, mate)]
        for half, part in enumerate(parts):
            pair_out[g][j][half] = part.astype(BF16)
            go(pair_copy(g, j, half), rows_of[g] * cuts_out[g][j][1])

    def keep(g, j):
        parts = [down(g, t, j) for t in (across, tp)]
        for which, part in enumerate(parts):
            own_part[g][j][which] = part

    def piece(g, i):
        off, size = cuts_back[g][i]
        for j, (base, wide) in enumerate(cuts_out[g]):
            if base <= off < base + wide:
                return j, slice(off - base, off - base + size)

    def cross(g, i):
        j, part = piece(g, i)
        if part.start == 0:
            pair_copy(g, j, 0).wait_recv()
        kept = own_part[g][j][0, :, part] + pair_in[g][j][0, :, part].astype(F32)
        cross_out[g][i][...] = kept.astype(BF16)
        go(tp_copy(cross_out[g][i], cross_in[g][i], ys_recv[g].at[i], across), rows_of[g] * cuts_back[g][i][1])

    def back(g, i):
        n = groups[g][1]
        j, part = piece(g, i)
        if part.start == 0:
            pair_copy(g, j, 1).wait_recv()
        near = own_part[g][j][1, :, part] + pair_in[g][j][1, :, part].astype(F32)
        tp_copy(cross_out[g][i], cross_in[g][i], ys_recv[g].at[i], across).wait_recv()
        total = ((near + cross_in[g][i][...].astype(F32)) * weight[g][...]).astype(BF16)
        if rows_of[g] == ep * n:
            back_out[g][i][...] = total
        else:
            wide = jnp.dot(spread[g][...], total, preferred_element_type=F32)
            back_out[g][i][...] = wide.astype(BF16)
        for c in ep_copies(back_out[g][i], back_in[g][i], n, back_recv[g].at[i]):
            go(c, n * cuts_back[g][i][1])
        back_in[g][i][mine_rows(n), :] = back_out[g][i][mine_rows(n), :]

    def finish(g, i):
        n = groups[g][1]
        off, size = cuts_back[g][i]
        landed(back_in[g][i], (ep - 1) * n, back_recv[g].at[i])
        part = jnp.dot(unpick[g][...], back_in[g][i][...], preferred_element_type=F32)
        if g:
            part = part + done[:, off : off + size]
        if g == n_groups - 1:
            out[:, off : off + size] = part.astype(BF16)
        else:
            done[:, off : off + size] = part

    def weights(i):
        loads[i].wait()

    start_on(0, (1, 0), (1, 1))
    recv(0, 0)
    start_on(1, (1, 0), (1, 1))
    recv(0, 1)
    start_on(0, (2, 0), (2, 1))
    weights(0)
    weights(1)
    project(0, [1], [], opening=True)
    recv(1, 0)
    start_on(1, (2, 0), (2, 1))
    project(0, [0], [])
    recv(1, 1)
    relay(0, 0)
    relay(0, 1)
    project(1, [0], [], opening=True)
    project(0, [], [0, 1], closing=True)
    recv(2, 0)
    weights(2)
    give(0, 0)
    recv(2, 1)
    relay(1, 0)
    keep(0, 0)
    relay(1, 1)
    cross(0, 0)
    project(1, [1], [0])
    cross(0, 1)
    project(1, [], [1], closing=True)
    give(1, 0)
    relay(2, 1)
    relay(2, 0)
    project(2, [1], [], opening=True)
    keep(1, 0)
    cross(1, 0)
    cross(1, 1)
    back(0, 0)
    project(2, [0], [0, 1], closing=True)
    give(2, 0)
    back(0, 1)
    keep(2, 0)
    cross(2, 0)
    back(1, 0)
    back(1, 1)
    cross(2, 1)
    back(2, 0)
    back(2, 1)
    finish(0, 0)
    finish(0, 1)
    finish(1, 0)
    finish(1, 1)
    finish(2, 0)
    finish(2, 1)

    words = sum(sent)
    rest = pl.ds(0, words // ff)
    pltpu.make_async_copy(gate_w.at[rest], gate_w.at[rest], send_sem.at[0]).wait()


def fused(tokens, norm_gain, chosen, route_weight, gate_weight, up_weight, down_weight):
    ep = lax.axis_size("ep")
    tok_rows, width = tokens.shape
    cap = chosen.shape[1]
    slots = 3 * tok_rows // 16
    quarter = width // lax.axis_size("tp")
    ff = gate_weight.shape[2]
    groups = cut(slots, SHARES)
    rows_of = [group_rows(cap, slots, ep, s0, n) for s0, n in groups]
    cuts_in = [cut(quarter, c) for c in CUTS_IN]
    cuts_out = [cut(quarter, c) for c in CUTS_OUT]
    cuts_back = [cut(quarter, c) for c in CUTS_BACK]
    hbm = pl.BlockSpec(memory_space=pl.ANY)
    dma = pltpu.SemaphoreType.DMA
    wide = [ep * n for _, n in groups]

    def bufs(cuts, lead, dtype=BF16):
        return [[pltpu.VMEM(lead(g) + (size,), dtype) for _, size in c] for g, c in enumerate(cuts)]

    def each(shape, dtype=BF16):
        return [pltpu.VMEM(shape(g), dtype) for g in range(len(groups))]

    def sems(cuts):
        return [dma((len(c),)) for c in cuts]

    return pl.pallas_call(
        functools.partial(fused_kernel, ep, groups, rows_of, cuts_in, cuts_out, cuts_back),
        out_shape=pltpu.VMEM((tok_rows, quarter), BF16),
        in_specs=[hbm] * 7,
        out_specs=pl.BlockSpec(memory_space=pltpu.VMEM),
        scratch_shapes=[
            pltpu.VMEM((tok_rows, width), BF16),
            pltpu.VMEM((1, width), F32),
            pltpu.VMEM(chosen.shape, jnp.int32),
            pltpu.VMEM((1, cap), F32),
            pltpu.VMEM((width, ff), BF16),
            pltpu.VMEM((width, ff), BF16),
            pltpu.VMEM((ff, width), BF16),
            pltpu.VMEM((tok_rows, quarter), BF16),
            each(lambda g: (wide[g], tok_rows), F32),
            each(lambda g: (tok_rows, wide[g])),
            each(lambda g: (wide[g], rows_of[g])),
            each(lambda g: (rows_of[g], wide[g])),
            each(lambda g: (rows_of[g], 1), F32),
            each(lambda g: (rows_of[g], ff), F32),
            each(lambda g: (rows_of[g], ff), F32),
            each(lambda g: (rows_of[g], ff)),
            bufs(cuts_in, lambda g: (wide[g],)),
            bufs(cuts_in, lambda g: (wide[g],)),
            bufs(cuts_in, lambda g: (4, rows_of[g])),
            bufs(cuts_out, lambda g: (2, rows_of[g])),
            bufs(cuts_out, lambda g: (2, rows_of[g])),
            bufs(cuts_out, lambda g: (2, rows_of[g]), F32),
            bufs(cuts_back, lambda g: (rows_of[g],)),
            bufs(cuts_back, lambda g: (rows_of[g],)),
            bufs(cuts_back, lambda g: (wide[g],)),
            bufs(cuts_back, lambda g: (wide[g],)),
            pltpu.VMEM((tok_rows, quarter), F32),
            dma((7,)),
            dma((3,)),
            dma((1,)),
            sems(cuts_in),
            sems(cuts_in),
            sems(cuts_in),
            sems(cuts_in),
            [dma((len(c), 2)) for c in cuts_out],
            sems(cuts_back),
            sems(cuts_back),
        ],
        compiler_params=pltpu.CompilerParams(
            collective_id=0, has_side_effects=True, vmem_limit_bytes=60 * 1024 * 1024,
        ),
    )(tokens, norm_gain[None, :], chosen, route_weight, gate_weight, up_weight, down_weight)


def solution(mesh):
    small = mesh.shape["tp"] == 4
    return jax.shard_map(
        fused if small else shards,
        mesh=mesh,
        in_specs=(
            P("ep", None),
            P(),
            P(),
            P("ep", None),
            P("ep", None, "tp"),
            P("ep", None, "tp"),
            P("ep", "tp", None),
        ),
        out_specs=P("ep", "tp"),
        check_vma=False,
    )
```
